32 devices in a mesh: ep: 8 (over z, core), tp: 4 (over y, x).
Axes of the slice: x: 2, y: 2, z: 4, core: 2. Of those that a mesh axis runs over, the one named last changes fastest.
Arguments:
- mixer_input: bfloat16 [2048, 1024], P('ep', 'tp'), may hold values from -6 to 6
- log_step: float32 [64], P('tp'), may hold values from -12.8 to -2.7
- decay_shift: float32 [2048, 64], P('ep', 'tp'), may hold values from -2 to 0
- input_map: bfloat16 [2, 64, 64, 16], P(None, 'tp'), may hold values from -71.55418 to 71.55418
- readout: float32 [2, 64, 16, 64], P(None, 'tp'), may hold values from -0.5 to 0.5
- mixer_weight: bfloat16 [1024, 2048], P(None, 'tp'), may hold values from -0.1875 to 0.1875
- expert_input: bfloat16 [1024, 2048], P('ep'), may hold values from -6 to 6
- norm_gain: float32 [2048], replicated, may hold values from 0.1 to 1.9
- routes: int32 [1024, 2], P('ep'), may hold values from 0 to 7, all different within a row; in each aligned block of 128 rows (0 to 127, 128 to 255, ...) at most 64 rows name the same one
- route_weight: float32 [1024, 2], P('ep'), may hold values from 0.1 to 2.5
- expert_switch_matrix: bfloat16 [8, 2048, 4096], P('ep', None, 'tp'), may hold values from -0.125 to 0.125
- up_weight: bfloat16 [8, 2048, 4096], P('ep', None, 'tp'), may hold values from -0.125 to 0.125
- down_weight: bfloat16 [8, 4096, 2048], P('ep', None, 'tp'), may hold values from -0.09375 to 0.09375
- shared_gate: bfloat16 [2048, 1024], P(None, 'tp'), may hold values from -0.125 to 0.125
- shared_up: bfloat16 [2048, 1024], P(None, 'tp'), may hold values from -0.125 to 0.125
- shared_down: bfloat16 [1024, 2048], P(None, 'tp'), may hold values from -0.1875 to 0.1875
Outputs:
- mixer_out: bfloat16 [2048, 2048], P('ep', 'tp')
- experts_out: bfloat16 [1024, 2048], P('ep', 'tp')
The draws below stay inside these ranges and needn't reach their ends.
Inputs may be any that keep to these rules, and one draw needn't show every extreme that they name: `routes`: each row names 2 different experts. In each aligned block of 128 rows (the rows of one index of ep) no expert is named by more than 64 rows, and in some block one expert is named by exactly 64 rows.
All inputs are finite; a program needn't handle non-finite values.
Results may differ from the reference program's by a relative error of at most 0.0069.
Values may be sent and summed in bfloat16 or wider, within the bound.
A program may use at most 128 MiB of HBM per device.

```python
import math
import jax
import jax.numpy as jnp
import numpy as np
from jax import lax

D = 2048
GROUPS = 64
GROUP = 16
STATE = 64
EXPERT_FF = 4096
FF = 1024
TOPK = 2
MIX_ROWS = 256
EXP_ROWS = 128
D_SSM = 1024
MIX_TOKENS = 2048
EXP_TOKENS = 1024
EXPERTS = 8
CAP = 64
N_EP = 8


def draw_steps(key):
    pick_key, fast_key, slow_key = jax.random.split(key, 3)
    quick = jax.random.randint(pick_key, (GROUPS,), 0, 2) < 1
    fast = jax.random.uniform(fast_key, (GROUPS,), jnp.float32, math.log(0.02), math.log(0.067))
    slow = jax.random.uniform(slow_key, (GROUPS,), jnp.float32, math.log(0.2), math.log(1.2)) - math.log(MIX_TOKENS)
    return jnp.where(quick, fast, slow)


def draw_log_step(key, part):
    return draw_steps(jax.random.fold_in(key, 101))


def draw_input_map(key, part):
    steps = draw_steps(jax.random.fold_in(key, 101))
    noise_key = jax.random.fold_in(key, 202)
    noise = jax.random.truncated_normal(noise_key, -4.0, 4.0, (2, GROUPS, STATE, GROUP), jnp.float32)
    scale = jnp.exp(-0.5 * steps)[None, :, None, None] / math.sqrt(2.0 * GROUP)
    return (noise * scale).astype(jnp.bfloat16)


def draw_decay_shift(key, part):
    rate_key, place_key, depth_key = jax.random.split(jax.random.fold_in(key, 303), 3)
    block_count = MIX_TOKENS // MIX_ROWS
    lowest, highest = (0.05, 0.4)
    block_rate = jnp.exp(jax.random.uniform(rate_key, (block_count, GROUPS), jnp.float32, math.log(lowest), math.log(highest))) / MIX_TOKENS
    shift_magnitude = -jnp.repeat(block_rate, MIX_ROWS, axis=0)
    capacity_indices = jax.random.randint(place_key, (2, GROUPS), 0, MIX_TOKENS)
    stack_levels = jnp.log(jax.random.uniform(depth_key, (2, GROUPS), jnp.float32, 0.55, 0.8))
    element_ordinals = jnp.arange(MIX_TOKENS, dtype=jnp.int32)[:, None, None]
    sequence_groupings = jnp.sum(jnp.where(element_ordinals == capacity_indices[None], stack_levels[None], 0.0), axis=1)
    return shift_magnitude + sequence_groupings


def steps_of(key, shape, pieces, least, high):
    def one(axis_at, blocks):
        steps = jax.random.uniform(jax.random.fold_in(jax.random.fold_in(key, 6), axis_at), (blocks,), jnp.float32, least / len(pieces), high / len(pieces))
        return jnp.repeat(jnp.exp(steps), shape[axis_at] // blocks).reshape((-1,) + (1,) * (len(shape) - axis_at - 1))

    level = one(*pieces[0])
    for cut in pieces[1:]:
        level = level * one(*cut)
    return level


def routed_block(key, own, number, rows, count, top, reach, slope):
    sequence = jax.random.permutation(key, count)
    crowded, common = load_shares(count, rows * top, reach, slope, True), load_shares(count, rows * top, reach, slope, False)
    places = jnp.arange(count)

    def named(tallies, turn):
        used = int((tallies > 0).sum())
        fixed = max(1, used // 4)
        shifted = fixed + (places - fixed + turn * (used - fixed)) % max(1, count - fixed)
        return jnp.zeros((count,), jnp.int32).at[sequence[jnp.where(places < fixed, places, shifted)]].set(jnp.asarray(tallies, jnp.int32))

    tallies = jnp.where(number % 4 == 0, named(crowded, number // 4), named(common, number - number // 4 - 1))
    mixed = jax.random.permutation(jax.random.fold_in(own, 3), count)
    donor, receiver = mixed[0:count // 2 * 2:2], mixed[1:count // 2 * 2:2]
    room = jnp.minimum(tallies[donor] - 1, reach - tallies[receiver]) // 2
    room = jnp.where((donor == sequence[0]) | (receiver == sequence[0]) | (tallies[receiver] == 0), 0, jnp.maximum(room, 0))
    shifted = jax.random.randint(jax.random.fold_in(own, 4), (count // 2,), 0, 1 << 20) % (room + 1)
    tallies = tallies.at[donor].add(-shifted).at[receiver].add(shifted)
    items = jnp.searchsorted(jnp.cumsum(tallies), jnp.arange(rows * top), side="right").astype(jnp.int32)
    table = items.reshape(top, rows).T
    table = table[jax.random.permutation(jax.random.fold_in(own, 1), rows)]
    turn = jax.random.randint(jax.random.fold_in(own, 2), (rows, 1), 0, top)
    return jnp.take_along_axis(table, (jnp.arange(top)[None, :] + turn) % top, axis=1)


def load_shares(amount, total, most, lean, full):
    weights = [(1 << 20) // math.isqrt(rank ** lean) + 1 for rank in range(1, amount + 1)]
    largest = most if full else min(most, max(-(-total // amount), total * weights[0] // sum(weights)))
    least = 1 if total - largest >= amount - 1 else 0
    holding, surplus = [largest] + [least] * (amount - 1), total - largest - least * (amount - 1)
    while surplus > 0:
        free = [i for i in range(1, amount) if holding[i] < largest] or [i for i in range(1, amount) if holding[i] < most]
        pool, remaining = sum([weights[i] for i in free]), surplus
        for i in free:
            addition = min(most - holding[i], max(1, remaining * weights[i] // pool), surplus)
            holding[i] = holding[i] + addition
            surplus = surplus - addition
    return np.array(holding)


def normal_values(key, shape, scale, bound, cuts=(), held_as=jnp.bfloat16):
    drawn = jax.random.normal(key, shape, jnp.float32) * scale
    if len(cuts) > 0:
        drawn = steps_of(key, shape, cuts, -0.22, 0.18) * drawn
    return jnp.clip(drawn, min=-bound, max=bound).astype(held_as)


def setup_inputs(seed: int = 0) -> dict:
    arg_keys = jax.random.split(jax.random.key(seed), 17)
    mixer_input = normal_values(arg_keys[0], (MIX_TOKENS, D_SSM), 1.0, 6.0, ((0, 8), (1, 4)))
    log_step = draw_log_step(jax.random.fold_in(arg_keys[16], 71), 0)
    decay_shift = draw_decay_shift(jax.random.fold_in(arg_keys[16], 71), 0)
    input_map = draw_input_map(jax.random.fold_in(arg_keys[16], 71), 0)
    readout = normal_values(arg_keys[4], (2, GROUPS, GROUP, STATE), (2 * STATE) ** -0.5, 0.5, ((1, 4),), jnp.float32)
    mixer_weight = normal_values(arg_keys[5], (D_SSM, D), D_SSM ** -0.5, 0.1875, ((1, 4),))
    expert_input = normal_values(arg_keys[6], (EXP_TOKENS, D), 1.0, 6.0, ((0, 8),))
    norm_gain = jnp.clip(1.0 + 0.18 * jax.random.normal(arg_keys[7], (D,), jnp.float32), 0.1, 1.9)
    routes_keys = jax.random.split(jax.random.fold_in(arg_keys[8], 1), EXP_TOKENS // EXP_ROWS)
    routes_turns = jax.random.permutation(jax.random.fold_in(arg_keys[8], 3), EXP_TOKENS // EXP_ROWS)
    routes = jax.vmap(lambda own, number: routed_block(jax.random.fold_in(arg_keys[8], 2), own, number, EXP_ROWS, EXPERTS, TOPK, CAP, 1))(routes_keys, routes_turns).reshape((EXP_TOKENS, TOPK))
    route_weight = jnp.clip(jnp.exp(math.log(2.5) - 3.218876 * jax.random.uniform(arg_keys[9], (EXP_TOKENS, TOPK), jnp.float32) ** steps_of(arg_keys[9], (EXP_TOKENS, TOPK), ((0, 8),), -0.2, 0.2)), 0.1, 2.5)
    expert_switch_matrix = normal_values(arg_keys[10], (EXPERTS, D, EXPERT_FF), D ** -0.5, 0.125, ((0, 8), (2, 4)))
    up_weight = normal_values(arg_keys[11], (EXPERTS, D, EXPERT_FF), D ** -0.5, 0.125, ((0, 8), (2, 4)))
    down_weight = normal_values(arg_keys[12], (EXPERTS, EXPERT_FF, D), EXPERT_FF ** -0.5, 0.09375, ((0, 8), (2, 4)))
    shared_gate = normal_values(arg_keys[13], (D, FF), D ** -0.5, 0.125, ((1, 4),))
    shared_up = normal_values(arg_keys[14], (D, FF), D ** -0.5, 0.125, ((1, 4),))
    shared_down = normal_values(arg_keys[15], (FF, D), FF ** -0.5, 0.1875, ((1, 4),))
    return {"mixer_input": mixer_input, "log_step": log_step, "decay_shift": decay_shift, "input_map": input_map, "readout": readout, "mixer_weight": mixer_weight, "expert_input": expert_input, "norm_gain": norm_gain, "routes": routes, "route_weight": route_weight, "expert_switch_matrix": expert_switch_matrix, "up_weight": up_weight, "down_weight": down_weight, "shared_gate": shared_gate, "shared_up": shared_up, "shared_down": shared_down}


def combine_parts(earlier, later):
    early_real, early_imaginary, early_shift_real, early_shift_imaginary = earlier
    late_real, late_imaginary, late_shift_real, late_shift_imaginary = later
    joint_real = late_real * early_real - late_imaginary * early_imaginary
    joint_imaginary = late_real * early_imaginary + late_imaginary * early_real
    shift_real = late_real * early_shift_real - late_imaginary * early_shift_imaginary + late_shift_real
    shift_imaginary = late_real * early_shift_imaginary + late_imaginary * early_shift_real + late_shift_imaginary
    return (joint_real, joint_imaginary, shift_real, shift_imaginary)

def factors(log_step, states):
    step_rate = jnp.exp(log_step)
    frequency = jnp.pi * jnp.arange(states, dtype=jnp.float32)
    angle = step_rate[:, None] * frequency[None, :]
    turn_cosine = jnp.cos(angle)
    turn_sine = jnp.sin(angle)
    base = jnp.exp(-0.5 * step_rate)[:, None]
    base_real = base * turn_cosine
    starting_quadrature = base * turn_sine
    inverse = 1.0 / (0.25 + frequency * frequency)[None, :]
    lowered = base_real - 1.0
    inject_real = (-0.5 * lowered + starting_quadrature * frequency[None, :]) * inverse
    inject_imaginary = (-0.5 * starting_quadrature - lowered * frequency[None, :]) * inverse
    return (step_rate, turn_cosine, turn_sine, inject_real, inject_imaginary)

def reference(mixer_input, log_step, decay_shift, input_map, readout, mixer_weight, expert_input, norm_gain, routes, route_weight, expert_switch_matrix, up_weight, down_weight, shared_gate, shared_up, shared_down):
    highest = lax.Precision.HIGHEST
    step_rate, turn_cosine, turn_sine, inject_real, inject_imaginary = factors(log_step, STATE)
    blocks_in = mixer_input.reshape(N_EP, MIX_ROWS, GROUPS, GROUP)
    blocks_shift = decay_shift.reshape(N_EP, MIX_ROWS, GROUPS)
    map_real = input_map[0].astype(jnp.float32)
    map_imaginary = input_map[1].astype(jnp.float32)

    def advance(carry, inputs):
        carry_real, carry_imaginary = carry
        block_in, block_shift = inputs
        magnitude = jnp.exp(-0.5 * step_rate[None, :] + block_shift)[:, :, None]
        decay_real = magnitude * turn_cosine[None]
        decay_imaginary = magnitude * turn_sine[None]
        values = block_in.astype(jnp.float32)
        drive_real = jnp.einsum('tgh,gph->tgp', values, map_real, precision=highest)
        drive_imaginary = jnp.einsum('tgh,gph->tgp', values, map_imaginary, precision=highest)
        push_real = inject_real[None] * drive_real - inject_imaginary[None] * drive_imaginary
        push_imaginary = inject_real[None] * drive_imaginary + inject_imaginary[None] * drive_real
        total_real, total_imaginary, local_real, local_imaginary = lax.associative_scan(combine_parts, (decay_real, decay_imaginary, push_real, push_imaginary), axis=0)
        state_real = local_real + total_real * carry_real[None] - total_imaginary * carry_imaginary[None]
        state_imaginary = local_imaginary + total_real * carry_imaginary[None] + total_imaginary * carry_real[None]
        mixed = jnp.einsum('ghp,tgp->tgh', readout[0], state_real, precision=highest) - jnp.einsum('ghp,tgp->tgh', readout[1], state_imaginary, precision=highest)
        return ((state_real[-1], state_imaginary[-1]), mixed.reshape(MIX_ROWS, GROUPS * GROUP))
    start = (jnp.zeros((GROUPS, STATE), jnp.float32), jnp.zeros((GROUPS, STATE), jnp.float32))
    _, outputs = lax.scan(advance, start, (blocks_in, blocks_shift))
    activated = jax.nn.gelu(outputs.reshape(MIX_TOKENS, GROUPS * GROUP)).astype(jnp.bfloat16)
    mixer_out = jnp.dot(activated, mixer_weight, preferred_element_type=jnp.float32).astype(jnp.bfloat16)
    values = expert_input.astype(jnp.float32)
    normed = (values * lax.rsqrt(lax.optimization_barrier(jnp.mean(values * values, axis=-1, keepdims=True)) + 1e-06) * norm_gain).astype(jnp.bfloat16)
    shared_hidden = (jax.nn.silu(jnp.dot(normed, shared_gate, preferred_element_type=jnp.float32)) * jnp.dot(normed, shared_up, preferred_element_type=jnp.float32)).astype(jnp.bfloat16)
    common_contribution = jnp.dot(shared_hidden, shared_down, preferred_element_type=jnp.float32)
    token_count = EXP_TOKENS
    limit = N_EP * CAP
    padded = jnp.concatenate([normed, jnp.zeros((1, D), jnp.bfloat16)], axis=0)

    def expert_step(total, expert):
        chosen = routes == expert
        member = jnp.any(chosen, axis=1)
        weight = lax.optimization_barrier(jnp.sum(jnp.where(chosen, route_weight, 0.0), axis=1))
        position = (jnp.cumsum(member.astype(jnp.int32)) - 1).astype(jnp.int32)
        target = jnp.where(member, position, limit).astype(jnp.int32)
        holder = jnp.full((limit,), token_count, jnp.int32).at[target].set(jnp.arange(token_count, dtype=jnp.int32), mode='drop')
        rows = padded[holder]
        hidden = (jax.nn.silu(jnp.dot(rows, expert_switch_matrix[expert], preferred_element_type=jnp.float32)) * jnp.dot(rows, up_weight[expert], preferred_element_type=jnp.float32)).astype(jnp.bfloat16)
        part = jnp.dot(hidden, down_weight[expert], preferred_element_type=jnp.float32).astype(jnp.bfloat16)
        scale = jnp.concatenate([weight, jnp.zeros((1,), jnp.float32)], axis=0)[holder]
        return (total.at[holder].add(part.astype(jnp.float32) * scale[:, None]), None)
    routed_output, _ = lax.scan(expert_step, jnp.zeros((token_count + 1, D), jnp.float32), jnp.arange(EXPERTS, dtype=jnp.int32))
    experts_out = (common_contribution + routed_output[:token_count]).astype(jnp.bfloat16)
    return (mixer_out, experts_out)
```

```python
import functools

import jax
import jax.numpy as jnp
from jax import lax
from jax.experimental import pallas as pl
from jax.experimental.pallas import tpu as pltpu
from jax.sharding import PartitionSpec as P

MESH = pl.DeviceIdType.MESH
SUBLANES = 8
NT = (((1,), (1,)), ((), ()))


def factors(log_step, states):
    step_rate = jnp.exp(log_step)
    frequency = jnp.pi * jnp.arange(states, dtype=jnp.float32)
    angle = step_rate[:, None] * frequency[None, :]
    turn_cosine = jnp.cos(angle)
    turn_sine = jnp.sin(angle)
    base = jnp.exp(-0.5 * step_rate)[:, None]
    base_real = base * turn_cosine
    starting_quadrature = base * turn_sine
    inverse = 1.0 / (0.25 + frequency * frequency)[None, :]
    lowered = base_real - 1.0
    inject_real = (-0.5 * lowered + starting_quadrature * frequency[None, :]) * inverse
    inject_imaginary = (-0.5 * starting_quadrature - lowered * frequency[None, :]) * inverse
    return (step_rate, turn_cosine, turn_sine, inject_real, inject_imaginary)


def times(ar, ai, br, bi):
    return ar * br - ai * bi, ar * bi + ai * br


def iota(shape, dim):
    return lax.broadcasted_iota(jnp.int32, shape, dim)


def spread(shape, period):
    return (iota(shape, 1) % period == iota(shape, 0)).astype(jnp.bfloat16)


def halves(a):
    high = a.astype(jnp.bfloat16)
    return high, (a - high.astype(jnp.float32)).astype(jnp.bfloat16)


def dot(a, b, dims=None):
    if dims is None:
        return jnp.dot(a, b, preferred_element_type=jnp.float32)
    return lax.dot_general(a, b, dims, preferred_element_type=jnp.float32)


def drive_into(x_ref, rate_ref, shift_ref, map_ref, table_ref, mag, push_re, push_im, states):
    rows, channels = x_ref.shape
    merged = mag.shape[1]
    groups = shift_ref.shape[1]
    width = channels // groups
    steps = rows // SUBLANES
    place = iota((rows, rows), 0)
    order = (iota((rows, rows), 1) == (place % SUBLANES) * steps + place // SUBLANES).astype(
        jnp.bfloat16
    )
    level = jnp.exp(-0.5 * jnp.exp(rate_ref[...]) + shift_ref[...])
    high, rest = halves(level)
    middle = rest
    low = ((level - high.astype(jnp.float32)) - middle.astype(jnp.float32)).astype(jnp.bfloat16)
    widen = (iota((groups, merged), 1) // states == iota((groups, merged), 0)).astype(jnp.bfloat16)
    total = None
    for piece in (high, middle, low):
        part = dot(dot(order, piece).astype(jnp.bfloat16), widen)
        total = part if total is None else total + part
    mag[...] = total
    x = dot(order, x_ref[...]).astype(jnp.bfloat16)
    repeat = spread((width, channels), width)
    mine = iota((merged, channels), 0) // states == iota((merged, channels), 1) // width
    drives = []
    for c in range(2):
        wide = jnp.where(mine, dot(map_ref[c], repeat), 0.0).astype(jnp.bfloat16)
        drives.append(dot(x, wide, NT))
    re, im = times(table_ref[2:3, :], table_ref[3:4, :], drives[0], drives[1])
    push_re[...] = re
    push_im[...] = im


def sweep(table_ref, mag, push_re, push_im, start_re, start_im, keep):
    rows, merged = mag.shape
    turn_re = jnp.broadcast_to(table_ref[0:1, :], (SUBLANES, merged))
    turn_im = jnp.broadcast_to(table_ref[1:2, :], (SUBLANES, merged))

    def one(j, carry):
        re, im, product = carry
        at = pl.ds(pl.multiple_of(j * SUBLANES, SUBLANES), SUBLANES)
        level = mag[at, :]
        next_re, next_im = times(turn_re, turn_im, re, im)
        next_re = level * next_re + push_re[at, :]
        next_im = level * next_im + push_im[at, :]
        if keep:
            push_re[at, :] = next_re
            push_im[at, :] = next_im
        else:
            product = product * level
        return next_re, next_im, product

    product = jnp.ones((SUBLANES, merged), jnp.float32)
    if keep:
        def pair(j, carry):
            return one(j, carry + (None,))[:2]
        return lax.fori_loop(0, rows // SUBLANES, pair, (start_re, start_im))
    return lax.fori_loop(0, rows // SUBLANES, one, (start_re, start_im, product))


def join(table_ref, ends_re, ends_im, product, pre, steps):
    merged = ends_re.shape[1]
    wr, wi = table_ref[0:1, :], table_ref[1:2, :]
    power = 1
    while power < steps:
        wr, wi = times(wr, wi, wr, wi)
        power *= 2
    cr = jnp.zeros((1, merged), jnp.float32)
    ci = cr
    ar = cr + 1.0
    ai = cr
    for s in range(SUBLANES):
        for i, v in enumerate((cr, ci, ar, ai)):
            pre[i, s : s + 1, :] = v
        level = product[s : s + 1]
        fr, fi = level * wr, level * wi
        tr, ti = times(fr, fi, cr, ci)
        cr, ci = tr + ends_re[s : s + 1], ti + ends_im[s : s + 1]
        ar, ai = times(fr, fi, ar, ai)
    return cr, ci, ar, ai


def read_states(readout_ref, push_re, push_im, states):
    rows, merged = push_re.shape
    channels = readout_ref.shape[1]
    width = channels * states // merged
    repeat = spread((states, merged), states)
    mine = iota((channels, merged), 1) // states == iota((channels, merged), 0) // width
    total = None
    for c, ref in enumerate((push_re, push_im)):
        high, low = halves(ref[...])
        back = readout_ref[c] if c == 0 else -readout_ref[c]
        wide_high, wide_low = (
            jnp.where(mine, dot(half, repeat), 0.0).astype(jnp.bfloat16) for half in halves(back)
        )
        part = dot(high, wide_high, NT) + (dot(low, wide_high, NT) + dot(high, wide_low, NT))
        total = part if total is None else total + part
    place = iota((rows, rows), 0)
    steps = rows // SUBLANES
    order = (iota((rows, rows), 1) == (place % steps) * SUBLANES + place // steps).astype(
        jnp.bfloat16
    )
    cube = total + 0.044715 * (total * total * total)
    active = (0.5 * total * (1.0 + jnp.tanh(0.7978845608028654 * cube))).astype(jnp.bfloat16)
    return dot(order, active).astype(jnp.bfloat16)


def mixer_kernel(
    n_ep, n_tp, states,
    x_ref, rate_ref, shift_ref, map_ref, readout_ref, table_ref, weight_ref,
    out_ref,
    mag, push_re, push_im, pre, summary, active,
    ep_send, ep_recv, tp_send, tp_recv,
):
    ep = lax.axis_index("ep")
    tp = lax.axis_index("tp")
    rows, channels = x_ref.shape
    merged = mag.shape[1]
    barrier = pltpu.get_barrier_semaphore()
    for d in range(1, n_ep):
        pl.semaphore_signal(
            barrier, inc=1, device_id={"ep": lax.rem(ep + d, n_ep)}, device_id_type=MESH
        )
    for d in range(1, n_tp):
        pl.semaphore_signal(
            barrier, inc=1, device_id={"tp": lax.rem(tp + d, n_tp)}, device_id_type=MESH
        )
    drive_into(x_ref, rate_ref, shift_ref, map_ref, table_ref, mag, push_re, push_im, states)
    zero = jnp.zeros((SUBLANES, merged), jnp.float32)
    ends_re, ends_im, product = sweep(table_ref, mag, push_re, push_im, zero, zero, False)
    end = join(table_ref, ends_re, ends_im, product, pre, rows // SUBLANES)
    for i, v in enumerate(end):
        summary[ep, i : i + 1, :] = v
    pl.semaphore_wait(barrier, n_ep + n_tp - 2)
    copies = []
    for d in range(1, n_ep):
        copy = pltpu.make_async_remote_copy(
            src_ref=summary.at[ep],
            dst_ref=summary.at[ep],
            send_sem=ep_send.at[d],
            recv_sem=ep_recv.at[d],
            device_id={"ep": lax.rem(ep + d, n_ep)},
            device_id_type=MESH,
        )
        copy.start()
        copies.append(copy)
    for copy in copies:
        copy.wait()

    def fold(e, carry):
        part = summary[e]
        re, im = times(part[2:3], part[3:4], carry[0], carry[1])
        return re + part[0:1], im + part[1:2]

    nothing = jnp.zeros((1, merged), jnp.float32)
    in_re, in_im = lax.fori_loop(0, ep, fold, (nothing, nothing))
    add_re, add_im = times(pre[2], pre[3], in_re, in_im)
    sweep(table_ref, mag, push_re, push_im, pre[0] + add_re, pre[1] + add_im, True)
    active[tp] = read_states(readout_ref, push_re, push_im, states)
    copies = []
    for d in range(1, n_tp):
        copy = pltpu.make_async_remote_copy(
            src_ref=active.at[tp],
            dst_ref=active.at[tp],
            send_sem=tp_send.at[d],
            recv_sem=tp_recv.at[d],
            device_id={"tp": lax.rem(tp + d, n_tp)},
            device_id_type=MESH,
        )
        copy.start()
        copies.append(copy)
    total = None
    for d in range(n_tp):
        if d > 0:
            copies[d - 1].wait()
        owner = lax.rem(tp + n_tp - d, n_tp)
        at = pl.ds(pl.multiple_of(owner * channels, channels), channels)
        part = dot(active[owner], weight_ref[at, :])
        total = part if total is None else total + part
    out_ref[...] = total.astype(out_ref.dtype)


def mixer(mixer_input, log_step, decay_shift, input_map, readout, mixer_weight):
    n_ep, n_tp = lax.axis_size("ep"), lax.axis_size("tp")
    rows, channels = mixer_input.shape
    groups = log_step.shape[0]
    states, width = input_map.shape[2:]
    merged = groups * states
    _, cosine, sine, inject_re, inject_im = factors(log_step, states)
    table = jnp.stack([a.reshape(merged) for a in (cosine, sine, inject_re, inject_im)])
    f32 = jnp.float32
    return pl.pallas_call(
        functools.partial(mixer_kernel, n_ep, n_tp, states),
        out_shape=jax.ShapeDtypeStruct((rows, mixer_weight.shape[1]), jnp.bfloat16),
        in_specs=[pl.BlockSpec(memory_space=pltpu.VMEM)] * 7,
        out_specs=pl.BlockSpec(memory_space=pltpu.VMEM),
        scratch_shapes=[
            pltpu.VMEM((rows, merged), f32),
            pltpu.VMEM((rows, merged), f32),
            pltpu.VMEM((rows, merged), f32),
            pltpu.VMEM((4, SUBLANES, merged), f32),
            pltpu.VMEM((n_ep, 4, merged), f32),
            pltpu.VMEM((n_tp, rows, channels), jnp.bfloat16),
            pltpu.SemaphoreType.DMA((n_ep,)),
            pltpu.SemaphoreType.DMA((n_ep,)),
            pltpu.SemaphoreType.DMA((n_tp,)),
            pltpu.SemaphoreType.DMA((n_tp,)),
        ],
        compiler_params=pltpu.CompilerParams(
            collective_id=0, has_side_effects=True, vmem_limit_bytes=40 * 1024 * 1024
        ),
        cost_estimate=pl.CostEstimate(
            flops=20_000_000_000, bytes_accessed=10_000_000, transcendentals=0
        ),
        name="mixer",
    )(
        mixer_input,
        log_step.reshape(1, groups),
        decay_shift,
        input_map.reshape(2, merged, width),
        readout.reshape(2, channels, states),
        table,
        mixer_weight,
    )


def shards(
    mixer_input,
    log_step,
    decay_shift,
    input_map,
    readout,
    mixer_weight,
    expert_input,
    norm_gain,
    routes,
    route_weight,
    expert_switch_matrix,
    up_weight,
    down_weight,
    shared_gate,
    shared_up,
    shared_down,
):
    mixer_out = mixer(mixer_input, log_step, decay_shift, input_map, readout, mixer_weight)
    token_count = expert_input.shape[0]
    features = expert_input.shape[1]
    top_count = routes.shape[1]
    experts = lax.axis_size("ep")
    capacity = 2 * token_count * top_count // experts
    values = expert_input.astype(jnp.float32)
    normed = (
        values * lax.rsqrt(jnp.mean(values * values, axis=-1, keepdims=True) + 1e-06) * norm_gain
    ).astype(jnp.bfloat16)
    flat_routes = routes.reshape(-1)
    onehot = (flat_routes[:, None] == jnp.arange(experts, dtype=jnp.int32)[None, :]).astype(
        jnp.int32
    )
    before = jnp.sum((jnp.cumsum(onehot, axis=0) - onehot) * onehot, axis=1)
    slot = flat_routes * capacity + before
    owner = jnp.arange(flat_routes.shape[0], dtype=jnp.int32) // top_count
    slot_token = jnp.full((experts * capacity,), token_count, jnp.int32).at[slot].set(owner)
    slice_width = down_weight.shape[2]
    received_rows = experts * capacity
    padded = jnp.concatenate([normed, jnp.zeros((1, features), jnp.bfloat16)], axis=0)
    outgoing = padded[slot_token].reshape(experts, capacity, features)
    arrived = lax.all_to_all(outgoing, "ep", split_axis=0, concat_axis=0, tiled=True).reshape(
        received_rows, features
    )
    gate_sum = jnp.dot(arrived, expert_switch_matrix[0], preferred_element_type=jnp.float32)
    up_sum = jnp.dot(arrived, up_weight[0], preferred_element_type=jnp.float32)
    expert_hidden = (jax.nn.silu(gate_sum) * up_sum).astype(jnp.bfloat16)
    shared_hidden = (
        jax.nn.silu(jnp.dot(normed, shared_gate, preferred_element_type=jnp.float32))
        * jnp.dot(normed, shared_up, preferred_element_type=jnp.float32)
    ).astype(jnp.bfloat16)
    rows_here = down_weight[0]
    routed_output = jnp.dot(
        lax.all_gather(expert_hidden, "tp", axis=1, tiled=True),
        rows_here,
        preferred_element_type=jnp.float32,
    )
    rows_here = shared_down
    common_contribution = jnp.dot(
        lax.all_gather(shared_hidden, "tp", axis=1, tiled=True),
        rows_here,
        preferred_element_type=jnp.float32,
    )
    returned = lax.all_to_all(
        routed_output.astype(jnp.bfloat16).reshape(experts, capacity, slice_width),
        "ep",
        split_axis=0,
        concat_axis=0,
        tiled=True,
    ).reshape(received_rows, slice_width)
    picked = returned[slot].reshape(token_count, top_count, slice_width).astype(jnp.float32)
    experts_out = (common_contribution + jnp.sum(route_weight[:, :, None] * picked, axis=1)).astype(
        jnp.bfloat16
    )
    return (mixer_out, experts_out)


def solution(mesh):
    placed = (
        P("ep", "tp"),
        P("tp"),
        P("ep", "tp"),
        P(None, "tp", None, None),
        P(None, "tp", None, None),
        P(None, "tp"),
        P("ep", None),
        P(),
        P("ep", None),
        P("ep", None),
        P("ep", None, "tp"),
        P("ep", None, "tp"),
        P("ep", None, "tp"),
        P(None, "tp"),
        P(None, "tp"),
        P(None, "tp"),
    )
    return jax.shard_map(
        shards,
        mesh=mesh,
        in_specs=placed,
        out_specs=(P("ep", "tp"), P("ep", "tp")),
        check_vma=False,
    )
```

```python
import functools

import jax
import jax.numpy as jnp
from jax import lax
from jax.experimental import pallas as pl
from jax.experimental.pallas import tpu as pltpu
from jax.sharding import PartitionSpec as P

MESH = pl.DeviceIdType.MESH
SUBLANES = 8
NT = (((1,), (1,)), ((), ()))


def factors(log_step, states):
    step_rate = jnp.exp(log_step)
    frequency = jnp.pi * jnp.arange(states, dtype=jnp.float32)
    angle = step_rate[:, None] * frequency[None, :]
    turn_cosine = jnp.cos(angle)
    turn_sine = jnp.sin(angle)
    base = jnp.exp(-0.5 * step_rate)[:, None]
    base_real = base * turn_cosine
    starting_quadrature = base * turn_sine
    inverse = 1.0 / (0.25 + frequency * frequency)[None, :]
    lowered = base_real - 1.0
    inject_real = (-0.5 * lowered + starting_quadrature * frequency[None, :]) * inverse
    inject_imaginary = (-0.5 * starting_quadrature - lowered * frequency[None, :]) * inverse
    return (step_rate, turn_cosine, turn_sine, inject_real, inject_imaginary)


def times(ar, ai, br, bi):
    return ar * br - ai * bi, ar * bi + ai * br


def iota(shape, dim):
    return lax.broadcasted_iota(jnp.int32, shape, dim)


def spread(shape, period):
    return (iota(shape, 1) % period == iota(shape, 0)).astype(jnp.bfloat16)


def halves(a):
    high = a.astype(jnp.bfloat16)
    return high, (a - high.astype(jnp.float32)).astype(jnp.bfloat16)


def dot(a, b, dims=None):
    if dims is None:
        return jnp.dot(a, b, preferred_element_type=jnp.float32)
    return lax.dot_general(a, b, dims, preferred_element_type=jnp.float32)


def drive_into(x_ref, rate_ref, shift_ref, map_ref, table_ref, mag, push_re, push_im, states):
    rows, channels = x_ref.shape
    merged = mag.shape[1]
    groups = shift_ref.shape[1]
    width = channels // groups
    steps = rows // SUBLANES
    place = iota((rows, rows), 0)
    order = (iota((rows, rows), 1) == (place % SUBLANES) * steps + place // SUBLANES).astype(
        jnp.bfloat16
    )
    level = jnp.exp(-0.5 * jnp.exp(rate_ref[...]) + shift_ref[...])
    high, rest = halves(level)
    middle = rest
    low = ((level - high.astype(jnp.float32)) - middle.astype(jnp.float32)).astype(jnp.bfloat16)
    widen = (iota((groups, merged), 1) // states == iota((groups, merged), 0)).astype(jnp.bfloat16)
    total = None
    for piece in (high, middle, low):
        part = dot(dot(order, piece).astype(jnp.bfloat16), widen)
        total = part if total is None else total + part
    mag[...] = total
    x = dot(order, x_ref[...]).astype(jnp.bfloat16)
    repeat = spread((width, channels), width)
    mine = iota((merged, channels), 0) // states == iota((merged, channels), 1) // width
    drives = []
    for c in range(2):
        wide = jnp.where(mine, dot(map_ref[c], repeat), 0.0).astype(jnp.bfloat16)
        drives.append(dot(x, wide, NT))
    re, im = times(table_ref[2:3, :], table_ref[3:4, :], drives[0], drives[1])
    push_re[...] = re
    push_im[...] = im


def sweep(table_ref, mag, push_re, push_im, start_re, start_im, keep):
    rows, merged = mag.shape
    turn_re = jnp.broadcast_to(table_ref[0:1, :], (SUBLANES, merged))
    turn_im = jnp.broadcast_to(table_ref[1:2, :], (SUBLANES, merged))

    def one(j, carry):
        re, im, product = carry
        at = pl.ds(pl.multiple_of(j * SUBLANES, SUBLANES), SUBLANES)
        level = mag[at, :]
        next_re, next_im = times(turn_re, turn_im, re, im)
        next_re = level * next_re + push_re[at, :]
        next_im = level * next_im + push_im[at, :]
        if keep:
            push_re[at, :] = next_re
            push_im[at, :] = next_im
        else:
            product = product * level
        return next_re, next_im, product

    product = jnp.ones((SUBLANES, merged), jnp.float32)
    if keep:
        def pair(j, carry):
            return one(j, carry + (None,))[:2]
        return lax.fori_loop(0, rows // SUBLANES, pair, (start_re, start_im))
    return lax.fori_loop(0, rows // SUBLANES, one, (start_re, start_im, product))


def join(table_ref, ends_re, ends_im, product, pre, steps):
    merged = ends_re.shape[1]
    wr, wi = table_ref[0:1, :], table_ref[1:2, :]
    power = 1
    while power < steps:
        wr, wi = times(wr, wi, wr, wi)
        power *= 2
    cr = jnp.zeros((1, merged), jnp.float32)
    ci = cr
    ar = cr + 1.0
    ai = cr
    for s in range(SUBLANES):
        for i, v in enumerate((cr, ci, ar, ai)):
            pre[i, s : s + 1, :] = v
        level = product[s : s + 1]
        fr, fi = level * wr, level * wi
        tr, ti = times(fr, fi, cr, ci)
        cr, ci = tr + ends_re[s : s + 1], ti + ends_im[s : s + 1]
        ar, ai = times(fr, fi, ar, ai)
    return cr, ci, ar, ai


def read_states(readout_ref, push_re, push_im, states):
    rows, merged = push_re.shape
    channels = readout_ref.shape[1]
    width = channels * states // merged
    repeat = spread((states, merged), states)
    mine = iota((channels, merged), 1) // states == iota((channels, merged), 0) // width
    total = None
    for c, ref in enumerate((push_re, push_im)):
        high, low = halves(ref[...])
        back = readout_ref[c] if c == 0 else -readout_ref[c]
        wide_high, wide_low = (
            jnp.where(mine, dot(half, repeat), 0.0).astype(jnp.bfloat16) for half in halves(back)
        )
        part = dot(high, wide_high, NT) + (dot(low, wide_high, NT) + dot(high, wide_low, NT))
        total = part if total is None else total + part
    place = iota((rows, rows), 0)
    steps = rows // SUBLANES
    order = (iota((rows, rows), 1) == (place % steps) * SUBLANES + place // steps).astype(
        jnp.bfloat16
    )
    cube = total + 0.044715 * (total * total * total)
    active = (0.5 * total * (1.0 + jnp.tanh(0.7978845608028654 * cube))).astype(jnp.bfloat16)
    return dot(order, active).astype(jnp.bfloat16)


def remote(src, dst, send, recv, **target):
    return pltpu.make_async_remote_copy(
        src_ref=src, dst_ref=dst, send_sem=send, recv_sem=recv,
        device_id=target, device_id_type=MESH,
    )


def fused_kernel(
    n_ep, n_tp, states,
    x_ref, rate_ref, shift_ref, map_ref, readout_ref, table_ref, weight_ref,
    outgoing, gains, normed, sgate_ref, sup_ref, sdown_ref, gate_hbm, up_hbm, down_hbm,
    out_ref, experts_ref,
    mag, push_re, push_im, pre, summary, active,
    gate, up, down, arrived, hidden, result, returned, shared,
    ep_send, ep_recv, tp_send, tp_recv,
    d_send, d_recv, h_send, h_recv, r_send, r_recv, s_send, s_recv, load,
):
    ep = lax.axis_index("ep")
    tp = lax.axis_index("tp")
    rows, channels = x_ref.shape
    merged = mag.shape[1]
    cap, features = outgoing.shape[1:]
    pair = hidden.shape[2] // cap
    chips = n_ep // pair
    chip = ep // pair
    ff = gate.shape[1]
    columns = down.shape[1]
    barrier = pltpu.get_barrier_semaphore()
    for d in range(1, n_ep):
        pl.semaphore_signal(
            barrier, inc=1, device_id={"ep": lax.rem(ep + d, n_ep)}, device_id_type=MESH
        )
    for d in range(1, n_tp):
        pl.semaphore_signal(
            barrier, inc=1, device_id={"tp": lax.rem(tp + d, n_tp)}, device_id_type=MESH
        )
    loads = [
        pltpu.make_async_copy(hbm.at[0], vmem, load.at[i])
        for i, (hbm, vmem) in enumerate(((gate_hbm, gate), (up_hbm, up), (down_hbm, down)))
    ]
    for copy in loads:
        copy.start()
    sends = []

    def go(copy):
        copy.start()
        sends.append(copy)

    drive_into(x_ref, rate_ref, shift_ref, map_ref, table_ref, mag, push_re, push_im, states)
    zero = jnp.zeros((SUBLANES, merged), jnp.float32)
    ends_re, ends_im, product = sweep(table_ref, mag, push_re, push_im, zero, zero, False)
    end = join(table_ref, ends_re, ends_im, product, pre, rows // SUBLANES)
    for i, v in enumerate(end):
        summary[ep, i : i + 1, :] = v
    pl.semaphore_wait(barrier, n_ep + n_tp - 2)
    carries = []
    for d in range(1, n_ep):
        copy = remote(
            summary.at[ep], summary.at[ep], ep_send.at[d], ep_recv.at[d],
            ep=lax.rem(ep + d, n_ep),
        )
        go(copy)
        carries.append(copy)
    others = [pair * chip + lax.rem(ep + c, pair) for c in range(1, pair)]
    for i in range(1, chips):
        others += [pair * lax.rem(chip + i, chips) + c for c in range(pair)]
    for target in others:
        go(remote(
            outgoing.at[target], arrived.at[ep], d_send.at[target], d_recv.at[ep], ep=target
        ))
    arrived[ep] = outgoing[ep]

    tokens = normed[...]
    v = dot(tokens, sgate_ref[...])
    shared[tp] = (v / (1.0 + jnp.exp(-v)) * dot(tokens, sup_ref[...])).astype(jnp.bfloat16)
    shares = []
    for d in range(1, n_tp):
        copy = remote(
            shared.at[tp], shared.at[tp], s_send.at[d], s_recv.at[d], tp=lax.rem(tp + d, n_tp)
        )
        go(copy)
        shares.append(copy)

    for copy in carries:
        copy.wait_recv()

    def fold(e, carry):
        part = summary[e]
        re, im = times(part[2:3], part[3:4], carry[0], carry[1])
        return re + part[0:1], im + part[1:2]

    nothing = jnp.zeros((1, merged), jnp.float32)
    in_re, in_im = lax.fori_loop(0, ep, fold, (nothing, nothing))
    add_re, add_im = times(pre[2], pre[3], in_re, in_im)
    sweep(table_ref, mag, push_re, push_im, pre[0] + add_re, pre[1] + add_im, True)
    active[tp] = read_states(readout_ref, push_re, push_im, states)
    mixes = []
    for d in range(1, n_tp):
        copy = remote(
            active.at[tp], active.at[tp], tp_send.at[d], tp_recv.at[d], tp=lax.rem(tp + d, n_tp)
        )
        go(copy)
        mixes.append(copy)
    for copy in loads:
        copy.wait()

    def project(i):
        there = lax.rem(chip + chips - i, chips)
        for d in range(1, n_tp):
            q = lax.rem(tp + d, n_tp)
            remote(
                hidden.at[there, q], hidden.at[there, q], h_send.at[there, q],
                h_recv.at[there, q], tp=q,
            ).wait_recv()
        total = None
        for q in range(n_tp):
            part = dot(hidden[there, q], down[q * ff : (q + 1) * ff, :])
            total = part if total is None else total + part
        result[there] = total.astype(jnp.bfloat16).reshape(pair, cap, columns)
        for c in range(pair):
            if i == 0 and c == 0:
                returned[ep] = result[there, lax.rem(ep, pair)]
                continue
            core = lax.rem(ep + c, pair) if i == 0 else c
            target = pair * there + core
            go(remote(
                result.at[there, core], returned.at[ep], r_send.at[target], r_recv.at[ep],
                ep=target,
            ))

    tile = min(ff, 256)
    for i in range(chips):
        there = lax.rem(chip + chips - i, chips)
        for c in range(pair):
            if i == 0 and c == 0:
                continue
            source = pair * there + (lax.rem(ep + c, pair) if i == 0 else c)
            remote(
                outgoing.at[source], arrived.at[source], d_send.at[source], d_recv.at[source],
                ep=source,
            ).wait_recv()
        block = pl.ds(pair * there, pair)

        @pl.loop(0, ff // tile)
        def _(n):
            at = pl.ds(pl.multiple_of(n * tile, tile), tile)
            a = arrived[block].reshape(pair * cap, features)
            v = dot(a, gate[:, at])
            hidden[there, tp, :, at] = (
                v / (1.0 + jnp.exp(-v)) * dot(a, up[:, at])
            ).astype(jnp.bfloat16)

        for d in range(1, n_tp):
            q = lax.rem(tp + d, n_tp)
            go(remote(
                hidden.at[there, tp], hidden.at[there, tp], h_send.at[there, q],
                h_recv.at[there, tp], tp=q,
            ))
        if i == 0:
            for copy in mixes:
                copy.wait_recv()
            total = None
            for q in range(n_tp):
                part = dot(active[q], weight_ref[q * channels : (q + 1) * channels, :])
                total = part if total is None else total + part
            out_ref[...] = total.astype(out_ref.dtype)
        else:
            project(i - 1)
    for copy in shares:
        copy.wait_recv()
    width = shared.shape[2]
    common = None
    for q in range(n_tp):
        part = dot(shared[q], sdown_ref[q * width : (q + 1) * width, :])
        common = part if common is None else common + part
    project(chips - 1)
    for source in others:
        remote(
            returned.at[source], returned.at[source], r_send.at[source], r_recv.at[source],
            ep=source,
        ).wait_recv()
    back = returned[...].reshape(n_ep * cap, columns)
    high, low = halves(gains[...])
    experts_ref[...] = (common + (dot(high, back) + dot(low, back))).astype(experts_ref.dtype)
    for copy in sends:
        copy.wait_send()


def shards(
    mixer_input,
    log_step,
    decay_shift,
    input_map,
    readout,
    mixer_weight,
    expert_input,
    norm_gain,
    routes,
    route_weight,
    expert_switch_matrix,
    up_weight,
    down_weight,
    shared_gate,
    shared_up,
    shared_down,
):
    n_ep, n_tp = lax.axis_size("ep"), lax.axis_size("tp")
    token_count, features = expert_input.shape
    top_count = routes.shape[1]
    cap = 2 * token_count * top_count // n_ep
    values = expert_input.astype(jnp.float32)
    normed = (
        values * lax.rsqrt(jnp.mean(values * values, axis=-1, keepdims=True) + 1e-06) * norm_gain
    ).astype(jnp.bfloat16)
    flat_routes = routes.reshape(-1)
    onehot = (flat_routes[:, None] == jnp.arange(n_ep, dtype=jnp.int32)[None, :]).astype(jnp.int32)
    before = jnp.sum((jnp.cumsum(onehot, axis=0) - onehot) * onehot, axis=1)
    slot = (flat_routes * cap + before).reshape(token_count, top_count)
    hit = slot[:, :, None] == jnp.arange(n_ep * cap, dtype=jnp.int32)[None, None, :]
    gains = jnp.sum(jnp.where(hit, route_weight[:, :, None], 0.0), axis=1)
    chosen = jnp.any(hit, axis=1).astype(jnp.bfloat16)
    outgoing = lax.dot_general(
        chosen, normed, (((0,), (0,)), ((), ())), preferred_element_type=jnp.float32
    ).astype(jnp.bfloat16).reshape(n_ep, cap, features)

    rows, channels = mixer_input.shape
    groups = log_step.shape[0]
    states, width = input_map.shape[2:]
    merged = groups * states
    _, cosine, sine, inject_re, inject_im = factors(log_step, states)
    table = jnp.stack([a.reshape(merged) for a in (cosine, sine, inject_re, inject_im)])
    f32, bf16 = jnp.float32, jnp.bfloat16
    pair = 2 if n_ep % 2 == 0 else 1
    chips = n_ep // pair
    ff = up_weight.shape[2]
    depth, columns = down_weight.shape[1:]
    vmem = pl.BlockSpec(memory_space=pltpu.VMEM)
    dma = pltpu.SemaphoreType.DMA
    return tuple(pl.pallas_call(
        functools.partial(fused_kernel, n_ep, n_tp, states),
        out_shape=(
            jax.ShapeDtypeStruct((rows, mixer_weight.shape[1]), bf16),
            jax.ShapeDtypeStruct((token_count, columns), bf16),
        ),
        in_specs=[vmem] * 13 + [pl.BlockSpec(memory_space=pl.ANY)] * 3,
        out_specs=(vmem, vmem),
        scratch_shapes=[
            pltpu.VMEM((rows, merged), f32),
            pltpu.VMEM((rows, merged), f32),
            pltpu.VMEM((rows, merged), f32),
            pltpu.VMEM((4, SUBLANES, merged), f32),
            pltpu.VMEM((n_ep, 4, merged), f32),
            pltpu.VMEM((n_tp, rows, channels), bf16),
            pltpu.VMEM((features, ff), bf16),
            pltpu.VMEM((features, ff), bf16),
            pltpu.VMEM((depth, columns), bf16),
            pltpu.VMEM((n_ep, cap, features), bf16),
            pltpu.VMEM((chips, n_tp, pair * cap, ff), bf16),
            pltpu.VMEM((chips, pair, cap, columns), bf16),
            pltpu.VMEM((n_ep, cap, columns), bf16),
            pltpu.VMEM((n_tp, token_count, shared_up.shape[1]), bf16),
            dma((n_ep,)), dma((n_ep,)), dma((n_tp,)), dma((n_tp,)),
            dma((n_ep,)), dma((n_ep,)), dma((chips, n_tp)), dma((chips, n_tp)),
            dma((n_ep,)), dma((n_ep,)), dma((n_tp,)), dma((n_tp,)), dma((3,)),
        ],
        compiler_params=pltpu.CompilerParams(
            collective_id=0, has_side_effects=True, vmem_limit_bytes=56 * 1024 * 1024
        ),
        name="fused",
    )(
        mixer_input,
        log_step.reshape(1, groups),
        decay_shift,
        input_map.reshape(2, merged, width),
        readout.reshape(2, channels, states),
        table,
        mixer_weight,
        outgoing,
        gains,
        normed,
        shared_gate,
        shared_up,
        shared_down,
        expert_switch_matrix,
        up_weight,
        down_weight,
    ))


def solution(mesh):
    placed = (
        P("ep", "tp"),
        P("tp"),
        P("ep", "tp"),
        P(None, "tp", None, None),
        P(None, "tp", None, None),
        P(None, "tp"),
        P("ep", None),
        P(),
        P("ep", None),
        P("ep", None),
        P("ep", None, "tp"),
        P("ep", None, "tp"),
        P("ep", None, "tp"),
        P(None, "tp"),
        P(None, "tp"),
        P(None, "tp"),
    )
    return jax.shard_map(
        shards,
        mesh=mesh,
        in_specs=placed,
        out_specs=(P("ep", "tp"), P("ep", "tp")),
        check_vma=False,
    )
```

```python
import functools

import jax
import jax.numpy as jnp
from jax import lax
from jax.experimental import pallas as pl
from jax.experimental.pallas import tpu as pltpu
from jax.sharding import PartitionSpec as P

MESH = pl.DeviceIdType.MESH
SUBLANES = 8
NT = (((1,), (1,)), ((), ()))


def factors(log_step, states):
    step_rate = jnp.exp(log_step)
    frequency = jnp.pi * jnp.arange(states, dtype=jnp.float32)
    angle = step_rate[:, None] * frequency[None, :]
    turn_cosine = jnp.cos(angle)
    turn_sine = jnp.sin(angle)
    base = jnp.exp(-0.5 * step_rate)[:, None]
    base_real = base * turn_cosine
    starting_quadrature = base * turn_sine
    inverse = 1.0 / (0.25 + frequency * frequency)[None, :]
    lowered = base_real - 1.0
    inject_real = (-0.5 * lowered + starting_quadrature * frequency[None, :]) * inverse
    inject_imaginary = (-0.5 * starting_quadrature - lowered * frequency[None, :]) * inverse
    return (step_rate, turn_cosine, turn_sine, inject_real, inject_imaginary)


def times(ar, ai, br, bi):
    return ar * br - ai * bi, ar * bi + ai * br


def iota(shape, dim):
    return lax.broadcasted_iota(jnp.int32, shape, dim)


def spread(shape, period):
    return (iota(shape, 1) % period == iota(shape, 0)).astype(jnp.bfloat16)


def halves(a):
    high = a.astype(jnp.bfloat16)
    return high, (a - high.astype(jnp.float32)).astype(jnp.bfloat16)


def dot(a, b, dims=None):
    if dims is None:
        return jnp.dot(a, b, preferred_element_type=jnp.float32)
    return lax.dot_general(a, b, dims, preferred_element_type=jnp.float32)


def drive_into(x_ref, rate_ref, shift_ref, map_ref, table_ref, mag, push_re, push_im, states):
    rows, channels = x_ref.shape
    merged = mag.shape[1]
    groups = shift_ref.shape[1]
    width = channels // groups
    steps = rows // SUBLANES
    place = iota((rows, rows), 0)
    order = (iota((rows, rows), 1) == (place % SUBLANES) * steps + place // SUBLANES).astype(
        jnp.bfloat16
    )
    level = jnp.exp(-0.5 * jnp.exp(rate_ref[...]) + shift_ref[...])
    high, rest = halves(level)
    middle = rest
    low = ((level - high.astype(jnp.float32)) - middle.astype(jnp.float32)).astype(jnp.bfloat16)
    widen = (iota((groups, merged), 1) // states == iota((groups, merged), 0)).astype(jnp.bfloat16)
    total = None
    for piece in (high, middle, low):
        part = dot(dot(order, piece).astype(jnp.bfloat16), widen)
        total = part if total is None else total + part
    mag[...] = total
    x = dot(order, x_ref[...]).astype(jnp.bfloat16)
    repeat = spread((width, channels), width)
    mine = iota((merged, channels), 0) // states == iota((merged, channels), 1) // width
    drives = []
    for c in range(2):
        wide = jnp.where(mine, dot(map_ref[c], repeat), 0.0).astype(jnp.bfloat16)
        drives.append(dot(x, wide, NT))
    re, im = times(table_ref[2:3, :], table_ref[3:4, :], drives[0], drives[1])
    push_re[...] = re
    push_im[...] = im


def sweep(table_ref, mag, push_re, push_im, start_re, start_im, keep):
    rows, merged = mag.shape
    turn_re = jnp.broadcast_to(table_ref[0:1, :], (SUBLANES, merged))
    turn_im = jnp.broadcast_to(table_ref[1:2, :], (SUBLANES, merged))

    def one(j, carry):
        re, im, product = carry
        at = pl.ds(pl.multiple_of(j * SUBLANES, SUBLANES), SUBLANES)
        level = mag[at, :]
        next_re, next_im = times(turn_re, turn_im, re, im)
        next_re = level * next_re + push_re[at, :]
        next_im = level * next_im + push_im[at, :]
        if keep:
            push_re[at, :] = next_re
            push_im[at, :] = next_im
        else:
            product = product * level
        return next_re, next_im, product

    product = jnp.ones((SUBLANES, merged), jnp.float32)
    if keep:
        def pair(j, carry):
            return one(j, carry + (None,))[:2]
        return lax.fori_loop(0, rows // SUBLANES, pair, (start_re, start_im))
    return lax.fori_loop(0, rows // SUBLANES, one, (start_re, start_im, product))


def join(table_ref, ends_re, ends_im, product, pre, steps):
    merged = ends_re.shape[1]
    wr, wi = table_ref[0:1, :], table_ref[1:2, :]
    power = 1
    while power < steps:
        wr, wi = times(wr, wi, wr, wi)
        power *= 2
    cr = jnp.zeros((1, merged), jnp.float32)
    ci = cr
    ar = cr + 1.0
    ai = cr
    for s in range(SUBLANES):
        for i, v in enumerate((cr, ci, ar, ai)):
            pre[i, s : s + 1, :] = v
        level = product[s : s + 1]
        fr, fi = level * wr, level * wi
        tr, ti = times(fr, fi, cr, ci)
        cr, ci = tr + ends_re[s : s + 1], ti + ends_im[s : s + 1]
        ar, ai = times(fr, fi, ar, ai)
    return cr, ci, ar, ai


def read_states(readout_ref, push_re, push_im, states):
    rows, merged = push_re.shape
    channels = readout_ref.shape[1]
    width = channels * states // merged
    repeat = spread((states, merged), states)
    mine = iota((channels, merged), 1) // states == iota((channels, merged), 0) // width
    total = None
    for c, ref in enumerate((push_re, push_im)):
        high, low = halves(ref[...])
        back = readout_ref[c] if c == 0 else -readout_ref[c]
        wide_high, wide_low = (
            jnp.where(mine, dot(half, repeat), 0.0).astype(jnp.bfloat16) for half in halves(back)
        )
        part = dot(high, wide_high, NT) + (dot(low, wide_high, NT) + dot(high, wide_low, NT))
        total = part if total is None else total + part
    place = iota((rows, rows), 0)
    steps = rows // SUBLANES
    order = (iota((rows, rows), 1) == (place % steps) * SUBLANES + place // steps).astype(
        jnp.bfloat16
    )
    cube = total + 0.044715 * (total * total * total)
    active = (0.5 * total * (1.0 + jnp.tanh(0.7978845608028654 * cube))).astype(jnp.bfloat16)
    return dot(order, active).astype(jnp.bfloat16)


def remote(src, dst, send, recv, **target):
    return pltpu.make_async_remote_copy(
        src_ref=src, dst_ref=dst, send_sem=send, recv_sem=recv,
        device_id=target, device_id_type=MESH,
    )


def fused_kernel(
    n_ep, n_tp, states,
    x_ref, rate_ref, shift_ref, map_ref, readout_ref, table_ref, weight_ref,
    outgoing, gains, normed, sgate_ref, sup_ref, sdown_ref, gate_hbm, up_hbm, down_hbm,
    out_ref, experts_ref,
    mag, push_re, push_im, pre, summary, active,
    gate, up, down, arrived, hidden, result, returned, shared,
    ep_send, ep_recv, tp_send, tp_recv,
    d_send, d_recv, h_send, h_recv, r_send, r_recv, s_send, s_recv, load,
):
    ep = lax.axis_index("ep")
    tp = lax.axis_index("tp")
    rows, channels = x_ref.shape
    merged = mag.shape[1]
    cap, features = outgoing.shape[1:]
    pair = hidden.shape[2] // cap
    chips = n_ep // pair
    chip = ep // pair
    ff = gate.shape[1]
    columns = down.shape[1]
    barrier = pltpu.get_barrier_semaphore()
    for d in range(1, n_ep):
        pl.semaphore_signal(
            barrier, inc=1, device_id={"ep": lax.rem(ep + d, n_ep)}, device_id_type=MESH
        )
    for d in range(1, n_tp):
        pl.semaphore_signal(
            barrier, inc=1, device_id={"tp": lax.rem(tp + d, n_tp)}, device_id_type=MESH
        )
    loads = [
        pltpu.make_async_copy(hbm.at[0], vmem, load.at[i])
        for i, (hbm, vmem) in enumerate(((gate_hbm, gate), (up_hbm, up), (down_hbm, down)))
    ]
    for copy in loads:
        copy.start()
    sends = []

    def go(copy):
        copy.start()
        sends.append(copy)

    pl.semaphore_wait(barrier, n_ep + n_tp - 2)
    others = [pair * chip + lax.rem(ep + c, pair) for c in range(1, pair)]
    for i in range(1, chips):
        others += [pair * lax.rem(chip + i, chips) + c for c in range(pair)]

    def dispatch(targets):
        for target in targets:
            go(remote(
                outgoing.at[target], arrived.at[ep], d_send.at[target], d_recv.at[ep], ep=target
            ))

    first = 2 * pair - 1
    dispatch(others[:first])
    drive_into(x_ref, rate_ref, shift_ref, map_ref, table_ref, mag, push_re, push_im, states)
    zero = jnp.zeros((SUBLANES, merged), jnp.float32)
    ends_re, ends_im, product = sweep(table_ref, mag, push_re, push_im, zero, zero, False)
    end = join(table_ref, ends_re, ends_im, product, pre, rows // SUBLANES)
    for i, v in enumerate(end):
        summary[ep, i : i + 1, :] = v
    carries = []
    for d in range(1, n_ep):
        copy = remote(
            summary.at[ep], summary.at[ep], ep_send.at[d], ep_recv.at[d],
            ep=lax.rem(ep + d, n_ep),
        )
        go(copy)
        carries.append(copy)
    dispatch(others[first:])
    arrived[ep] = outgoing[ep]

    tokens = normed[...]
    v = dot(tokens, sgate_ref[...])
    shared[tp] = (v / (1.0 + jnp.exp(-v)) * dot(tokens, sup_ref[...])).astype(jnp.bfloat16)
    shares = []
    for d in range(1, n_tp):
        copy = remote(
            shared.at[tp], shared.at[tp], s_send.at[d], s_recv.at[d], tp=lax.rem(tp + d, n_tp)
        )
        go(copy)
        shares.append(copy)

    tile = min(ff, 256)

    def expand(i):
        there = lax.rem(chip + chips - i, chips)
        for c in range(pair):
            if i == 0 and c == 0:
                continue
            source = pair * there + (lax.rem(ep + c, pair) if i == 0 else c)
            remote(
                outgoing.at[source], arrived.at[source], d_send.at[source], d_recv.at[source],
                ep=source,
            ).wait_recv()
        block = pl.ds(pair * there, pair)

        @pl.loop(0, ff // tile)
        def _(n):
            at = pl.ds(pl.multiple_of(n * tile, tile), tile)
            a = arrived[block].reshape(pair * cap, features)
            v = dot(a, gate[:, at])
            hidden[there, tp, :, at] = (
                v / (1.0 + jnp.exp(-v)) * dot(a, up[:, at])
            ).astype(jnp.bfloat16)

        for d in range(1, n_tp):
            q = lax.rem(tp + d, n_tp)
            go(remote(
                hidden.at[there, tp], hidden.at[there, tp], h_send.at[there, q],
                h_recv.at[there, tp], tp=q,
            ))

    for copy in loads[:2]:
        copy.wait()
    expand(0)
    for copy in carries:
        copy.wait_recv()

    def fold(e, carry):
        part = summary[e]
        re, im = times(part[2:3], part[3:4], carry[0], carry[1])
        return re + part[0:1], im + part[1:2]

    nothing = jnp.zeros((1, merged), jnp.float32)
    in_re, in_im = lax.fori_loop(0, ep, fold, (nothing, nothing))
    add_re, add_im = times(pre[2], pre[3], in_re, in_im)
    sweep(table_ref, mag, push_re, push_im, pre[0] + add_re, pre[1] + add_im, True)
    active[tp] = read_states(readout_ref, push_re, push_im, states)
    mixes = []
    for d in range(1, n_tp):
        copy = remote(
            active.at[tp], active.at[tp], tp_send.at[d], tp_recv.at[d], tp=lax.rem(tp + d, n_tp)
        )
        go(copy)
        mixes.append(copy)
    def project(i):
        there = lax.rem(chip + chips - i, chips)
        for d in range(1, n_tp):
            q = lax.rem(tp + d, n_tp)
            remote(
                hidden.at[there, q], hidden.at[there, q], h_send.at[there, q],
                h_recv.at[there, q], tp=q,
            ).wait_recv()
        total = None
        for q in range(n_tp):
            part = dot(hidden[there, q], down[q * ff : (q + 1) * ff, :])
            total = part if total is None else total + part
        result[there] = total.astype(jnp.bfloat16).reshape(pair, cap, columns)
        for c in range(pair):
            if i == 0 and c == 0:
                returned[ep] = result[there, lax.rem(ep, pair)]
                continue
            core = lax.rem(ep + c, pair) if i == 0 else c
            target = pair * there + core
            go(remote(
                result.at[there, core], returned.at[ep], r_send.at[target], r_recv.at[ep],
                ep=target,
            ))

    for copy in loads[2:]:
        copy.wait()
    for i in range(1, chips):
        expand(i)
        project(i - 1)
    for copy in mixes:
        copy.wait_recv()
    total = None
    for q in range(n_tp):
        part = dot(active[q], weight_ref[q * channels : (q + 1) * channels, :])
        total = part if total is None else total + part
    out_ref[...] = total.astype(out_ref.dtype)
    for copy in shares:
        copy.wait_recv()
    width = shared.shape[2]
    common = None
    for q in range(n_tp):
        part = dot(shared[q], sdown_ref[q * width : (q + 1) * width, :])
        common = part if common is None else common + part
    project(chips - 1)
    for source in others:
        remote(
            returned.at[source], returned.at[source], r_send.at[source], r_recv.at[source],
            ep=source,
        ).wait_recv()
    back = returned[...].reshape(n_ep * cap, columns)
    high, low = halves(gains[...])
    experts_ref[...] = (common + (dot(high, back) + dot(low, back))).astype(experts_ref.dtype)
    for copy in sends:
        copy.wait_send()


def shards(
    mixer_input,
    log_step,
    decay_shift,
    input_map,
    readout,
    mixer_weight,
    expert_input,
    norm_gain,
    routes,
    route_weight,
    expert_switch_matrix,
    up_weight,
    down_weight,
    shared_gate,
    shared_up,
    shared_down,
):
    n_ep, n_tp = lax.axis_size("ep"), lax.axis_size("tp")
    token_count, features = expert_input.shape
    top_count = routes.shape[1]
    cap = 2 * token_count * top_count // n_ep
    values = expert_input.astype(jnp.float32)
    normed = (
        values * lax.rsqrt(jnp.mean(values * values, axis=-1, keepdims=True) + 1e-06) * norm_gain
    ).astype(jnp.bfloat16)
    flat_routes = routes.reshape(-1)
    onehot = (flat_routes[:, None] == jnp.arange(n_ep, dtype=jnp.int32)[None, :]).astype(jnp.int32)
    before = jnp.sum((jnp.cumsum(onehot, axis=0) - onehot) * onehot, axis=1)
    slot = (flat_routes * cap + before).reshape(token_count, top_count)
    hit = slot[:, :, None] == jnp.arange(n_ep * cap, dtype=jnp.int32)[None, None, :]
    gains = jnp.sum(jnp.where(hit, route_weight[:, :, None], 0.0), axis=1)
    chosen = jnp.any(hit, axis=1).astype(jnp.bfloat16)
    outgoing = lax.dot_general(
        chosen, normed, (((0,), (0,)), ((), ())), preferred_element_type=jnp.float32
    ).astype(jnp.bfloat16).reshape(n_ep, cap, features)

    rows, channels = mixer_input.shape
    groups = log_step.shape[0]
    states, width = input_map.shape[2:]
    merged = groups * states
    _, cosine, sine, inject_re, inject_im = factors(log_step, states)
    table = jnp.stack([a.reshape(merged) for a in (cosine, sine, inject_re, inject_im)])
    f32, bf16 = jnp.float32, jnp.bfloat16
    pair = 2 if n_ep % 2 == 0 else 1
    chips = n_ep // pair
    ff = up_weight.shape[2]
    depth, columns = down_weight.shape[1:]
    vmem = pl.BlockSpec(memory_space=pltpu.VMEM)
    dma = pltpu.SemaphoreType.DMA
    return tuple(pl.pallas_call(
        functools.partial(fused_kernel, n_ep, n_tp, states),
        out_shape=(
            jax.ShapeDtypeStruct((rows, mixer_weight.shape[1]), bf16),
            jax.ShapeDtypeStruct((token_count, columns), bf16),
        ),
        in_specs=[vmem] * 13 + [pl.BlockSpec(memory_space=pl.ANY)] * 3,
        out_specs=(vmem, vmem),
        scratch_shapes=[
            pltpu.VMEM((rows, merged), f32),
            pltpu.VMEM((rows, merged), f32),
            pltpu.VMEM((rows, merged), f32),
            pltpu.VMEM((4, SUBLANES, merged), f32),
            pltpu.VMEM((n_ep, 4, merged), f32),
            pltpu.VMEM((n_tp, rows, channels), bf16),
            pltpu.VMEM((features, ff), bf16),
            pltpu.VMEM((features, ff), bf16),
            pltpu.VMEM((depth, columns), bf16),
            pltpu.VMEM((n_ep, cap, features), bf16),
            pltpu.VMEM((chips, n_tp, pair * cap, ff), bf16),
            pltpu.VMEM((chips, pair, cap, columns), bf16),
            pltpu.VMEM((n_ep, cap, columns), bf16),
            pltpu.VMEM((n_tp, token_count, shared_up.shape[1]), bf16),
            dma((n_ep,)), dma((n_ep,)), dma((n_tp,)), dma((n_tp,)),
            dma((n_ep,)), dma((n_ep,)), dma((chips, n_tp)), dma((chips, n_tp)),
            dma((n_ep,)), dma((n_ep,)), dma((n_tp,)), dma((n_tp,)), dma((3,)),
        ],
        compiler_params=pltpu.CompilerParams(
            collective_id=0, has_side_effects=True, vmem_limit_bytes=56 * 1024 * 1024
        ),
        name="fused",
    )(
        mixer_input,
        log_step.reshape(1, groups),
        decay_shift,
        input_map.reshape(2, merged, width),
        readout.reshape(2, channels, states),
        table,
        mixer_weight,
        outgoing,
        gains,
        normed,
        shared_gate,
        shared_up,
        shared_down,
        expert_switch_matrix,
        up_weight,
        down_weight,
    ))


def solution(mesh):
    placed = (
        P("ep", "tp"),
        P("tp"),
        P("ep", "tp"),
        P(None, "tp", None, None),
        P(None, "tp", None, None),
        P(None, "tp"),
        P("ep", None),
        P(),
        P("ep", None),
        P("ep", None),
        P("ep", None, "tp"),
        P("ep", None, "tp"),
        P("ep", None, "tp"),
        P(None, "tp"),
        P(None, "tp"),
        P(None, "tp"),
    )
    return jax.shard_map(
        shards,
        mesh=mesh,
        in_specs=placed,
        out_specs=(P("ep", "tp"), P("ep", "tp")),
        check_vma=False,
    )
```
